128 devices in a mesh: kv: 16 (over z, y), tp: 8 (over x, core).
Axes of the slice: x: 4, y: 4, z: 4, core: 2. Of those that a mesh axis runs over, the one named last changes fastest.
Arguments:
- tokens: bfloat16 [320, 4096], P(None, 'kv'), may hold values from -40 to 40
- input_norm_gain: float32 [4096], P('kv'), may hold values from 0.1 to 1.9
- input_matrix: bfloat16 [4096, 4096], P('kv', 'tp'), may hold values from -0.09375 to 0.09375
- gate_matrix: bfloat16 [4096, 4096], P('kv', 'tp'), may hold values from -0.09375 to 0.09375
- write_matrix: bfloat16 [4096, 1024], P('kv', 'tp'), may hold values from -0.09375 to 0.09375
- read_matrix: bfloat16 [4096, 1024], P('kv', 'tp'), may hold values from -0.09375 to 0.09375
- step_matrix: bfloat16 [4096, 64], replicated, may hold values from -0.09375 to 0.09375
- input_kernel: float32 [4, 4096], P(None, 'tp'), may hold values from -3 to 3
- write_kernel: float32 [4, 1024], P(None, 'tp'), may hold values from -3 to 3
- read_kernel: float32 [4, 1024], P(None, 'tp'), may hold values from -3 to 3
- step_size_bias: float32 [64], P('tp'), may hold values from -6 to 1
- head_decay_logs: float32 [64], P('tp'), may hold values from 0 to 2.77
- bypass_scale: float32 [64], P('tp'), may hold values from 0.5 to 1.5
- extra_decay_logs: float32 [320, 64], P('kv', 'tp'), may hold values from -0.7 to 0, as said below
- output_norm_gain: float32 [4096], P('tp'), may hold values from 0.1 to 1.9
- output_matrix: bfloat16 [4096, 4096], P('tp', 'kv'), may hold values from -0.09375 to 0.09375
- cached_state_history: float32 [64, 6, 64, 64, 128], P('kv', None, 'tp'), may hold values from -2 to 2
- cached_input_rows: bfloat16 [64, 8, 4096], P('kv', None, 'tp'), may hold values from -6 to 6
- cached_write_rows: bfloat16 [64, 8, 1024], P('kv', None, 'tp'), may hold values from -6 to 6
- cached_read_rows: bfloat16 [64, 8, 1024], P('kv', None, 'tp'), may hold values from -6 to 6
- accepted: int32 [64], P('kv'), may hold values from 0 to 5
Outputs:
- mixer_out: bfloat16 [320, 4096], P('tp', 'kv')
- next_states: float32 [64, 6, 64, 64, 128], P('kv', None, 'tp')
- next_input: bfloat16 [64, 8, 4096], P('kv', None, 'tp')
- next_write: bfloat16 [64, 8, 1024], P('kv', None, 'tp')
- next_read: bfloat16 [64, 8, 1024], P('kv', None, 'tp')
The draws below stay inside these ranges and needn't reach their ends.
Inputs may be any that keep to these rules, and one draw needn't show every extreme that they name: `extra_decay_logs`: zero at most tokens and heads.
All inputs are finite; a program needn't handle non-finite values.
Results may differ from the reference program's by a relative error of at most 0.03.
Values may be sent and summed in bfloat16 or wider, within the bound.
No kernel may reach another device: no remote copies, remote signals or barrier semaphores. Data moves between devices by JAX's collectives and lax.ppermute only.
A program may use at most 64 MiB of HBM per device.

```python
import math
import jax
import jax.numpy as jnp
from jax import lax

D = 4096
HEAD_TOTAL = 64
P_SIZE = 64
N = 128
G = 8
TAPS = 4
DRAFT_TOKENS = 5
SEQUENCE_TOTAL = 64
TOKENS = 320
N_TP = 8


def draw_tokens(key, part):
    first, second, third = jax.random.split(jax.random.fold_in(key, 11), 3)
    column = jnp.arange(D, dtype=jnp.float32)
    column_scale = jnp.exp(math.log(3.0) * column / max(D - 1, 1)) * jnp.exp(jax.random.uniform(second, (D,), jnp.float32, -0.35, 0.35))
    base = jax.random.normal(first, (TOKENS, D), jnp.float32)
    row_scale = jnp.exp(jax.random.uniform(third, (TOKENS, 1), jnp.float32, math.log(0.3), math.log(3.0)))
    values = jnp.clip(base * row_scale * column_scale[None, :], -40.0, 40.0)
    return values.astype(jnp.bfloat16)


def draw_extra_decay_logs(key, part):
    first, second = jax.random.split(jax.random.fold_in(key, 23), 2)
    struck = jax.random.randint(first, (TOKENS, HEAD_TOTAL), 0, 4) == 0
    depth = jax.random.uniform(second, (TOKENS, HEAD_TOTAL), jnp.float32, -0.5, -0.22)
    return jnp.where(struck, depth, 0.0).astype(jnp.float32)


def touch_ends(result, key, low, high):
    longest = result.shape.index(max(result.shape))
    spots = []
    for shift in (0, 1):
        where = [jax.random.randint(jax.random.fold_in(key, axis), (), 0, length) for axis, length in enumerate(result.shape)]
        where[longest] = (where[longest] + shift) % result.shape[longest]
        spots.append(tuple(where))
    return result.at[spots[0]].set(low).at[spots[1]].set(high)


def block_levels(rng, dims, cuts, low, top_value):
    gain = 1.0
    for dim, parts in cuts:
        draws = jax.random.uniform(jax.random.fold_in(jax.random.fold_in(rng, 6), dim), (parts,), jnp.float32, low / len(cuts), top_value / len(cuts))
        gain = gain * jnp.repeat(jnp.exp(draws), dims[dim] // parts).reshape((-1,) + (1,) * (len(dims) - 1 - dim))
    return gain


def gaussian(own_key, extent, width, reach, cuts=(), kind=jnp.bfloat16):
    values = jax.random.normal(own_key, extent, jnp.float32) * width
    if len(cuts) > 0:
        values = block_levels(own_key, extent, cuts, -0.22, 0.18) * values
    return jnp.clip(values, min=-reach, max=reach).astype(kind)


def setup_inputs(seed: int = 0) -> dict:
    key_list = jax.random.split(jax.random.key(seed), 22)
    return {
        "tokens": draw_tokens(jax.random.fold_in(key_list[21], 71), 0),
        "input_norm_gain": jnp.clip(1.0 + 0.18 * jax.random.normal(key_list[1], (D,), jnp.float32), 0.1, 1.9),
        "input_matrix": gaussian(key_list[2], (D, HEAD_TOTAL * P_SIZE), D ** -0.5, 0.09375, ((0, 16), (1, 8))),
        "gate_matrix": gaussian(key_list[3], (D, HEAD_TOTAL * P_SIZE), D ** -0.5, 0.09375, ((0, 16), (1, 8))),
        "write_matrix": gaussian(key_list[4], (D, G * N), D ** -0.5, 0.09375, ((0, 16), (1, 8))),
        "read_matrix": gaussian(key_list[5], (D, G * N), D ** -0.5, 0.09375, ((0, 16), (1, 8))),
        "step_matrix": gaussian(key_list[6], (D, HEAD_TOTAL), D ** -0.5, 0.09375),
        "input_kernel": gaussian(key_list[7], (TAPS, HEAD_TOTAL * P_SIZE), 0.5, 3.0, ((1, 8),), jnp.float32),
        "write_kernel": gaussian(key_list[8], (TAPS, G * N), 0.5, 3.0, ((1, 8),), jnp.float32),
        "read_kernel": gaussian(key_list[9], (TAPS, G * N), 0.5, 3.0, ((1, 8),), jnp.float32),
        "step_size_bias": jnp.clip(-6.0 + 7.0 * jax.random.uniform(key_list[10], (HEAD_TOTAL,), jnp.float32) ** block_levels(key_list[10], (HEAD_TOTAL,), ((0, 8),), -0.2, 0.2), -6.0, 1.0),
        "head_decay_logs": jnp.clip(2.77 * jax.random.uniform(key_list[11], (HEAD_TOTAL,), jnp.float32) ** block_levels(key_list[11], (HEAD_TOTAL,), ((0, 8),), -0.2, 0.2), 0.0, 2.77),
        "bypass_scale": jnp.clip(0.5 + 1.0 * jax.random.uniform(key_list[12], (HEAD_TOTAL,), jnp.float32) ** block_levels(key_list[12], (HEAD_TOTAL,), ((0, 8),), -0.2, 0.2), 0.5, 1.5),
        "extra_decay_logs": draw_extra_decay_logs(jax.random.fold_in(key_list[21], 71), 0),
        "output_norm_gain": jnp.clip(1.0 + 0.18 * jax.random.normal(key_list[14], (HEAD_TOTAL * P_SIZE,), jnp.float32), 0.1, 1.9),
        "output_matrix": gaussian(key_list[15], (HEAD_TOTAL * P_SIZE, D), (HEAD_TOTAL * P_SIZE) ** -0.5, 0.09375, ((0, 8), (1, 16))),
        "cached_state_history": gaussian(key_list[16], (SEQUENCE_TOTAL, DRAFT_TOKENS + 1, HEAD_TOTAL, P_SIZE, N), 0.3, 2.0, ((0, 16), (2, 8)), jnp.float32),
        "cached_input_rows": gaussian(key_list[17], (SEQUENCE_TOTAL, DRAFT_TOKENS + TAPS - 1, HEAD_TOTAL * P_SIZE), 1.0, 6.0, ((0, 16), (2, 8))),
        "cached_write_rows": gaussian(key_list[18], (SEQUENCE_TOTAL, DRAFT_TOKENS + TAPS - 1, G * N), 1.0, 6.0, ((0, 16), (2, 8))),
        "cached_read_rows": gaussian(key_list[19], (SEQUENCE_TOTAL, DRAFT_TOKENS + TAPS - 1, G * N), 1.0, 6.0, ((0, 16), (2, 8))),
        "accepted": touch_ends(jax.random.randint(key_list[20], (SEQUENCE_TOTAL,), 0, DRAFT_TOKENS + 1), jax.random.fold_in(key_list[20], 1), 0, DRAFT_TOKENS).astype(jnp.int32),
    }


epsilon = 1e-05

def make_window(saved, fresh, accepted):
    offsets = jnp.arange(TAPS - 1, dtype=jnp.int32)
    index = (accepted[:, None] + offsets[None, :]).astype(jnp.int32)
    taken_rows = jnp.take_along_axis(saved, index[:, :, None], axis=1)
    return jnp.concatenate([taken_rows, fresh.reshape(SEQUENCE_TOTAL, DRAFT_TOKENS, -1)], axis=1)

def convolve(window, taps):
    total = jnp.zeros((window.shape[0], DRAFT_TOKENS, window.shape[2]), jnp.float32)
    for tap_index in range(TAPS):
        total = total + taps[tap_index] * window[:, tap_index:tap_index + DRAFT_TOKENS].astype(jnp.float32)
    return jax.nn.silu(total)

def reference(tokens, input_norm_gain, input_matrix, gate_matrix, write_matrix, read_matrix, step_matrix, input_kernel, write_kernel, read_kernel, step_size_bias, head_decay_logs, bypass_scale, extra_decay_logs, output_norm_gain, output_matrix, cached_state_history, cached_input_rows, cached_write_rows, cached_read_rows, accepted):
    wide_rows = tokens.astype(jnp.float32)
    inverse = lax.rsqrt(lax.optimization_barrier(jnp.sum(wide_rows * wide_rows, axis=1, keepdims=True)) / D + epsilon)
    scaled = (wide_rows * input_norm_gain).astype(jnp.bfloat16)

    def project(weight):
        return (jnp.dot(scaled, weight, preferred_element_type=jnp.float32) * inverse).astype(jnp.bfloat16)
    fresh_input = project(input_matrix)
    fresh_gate = project(gate_matrix)
    fresh_write = project(write_matrix)
    fresh_read = project(read_matrix)
    step_raw = jnp.dot(scaled, step_matrix, preferred_element_type=jnp.float32) * inverse
    next_input = make_window(cached_input_rows, fresh_input, accepted)
    next_write = make_window(cached_write_rows, fresh_write, accepted)
    next_read = make_window(cached_read_rows, fresh_read, accepted)
    conv_input = convolve(next_input, input_kernel).reshape(SEQUENCE_TOTAL, DRAFT_TOKENS, HEAD_TOTAL, P_SIZE)
    conv_write = jnp.repeat(convolve(next_write, write_kernel).reshape(SEQUENCE_TOTAL, DRAFT_TOKENS, G, N), HEAD_TOTAL // G, axis=2)
    conv_read = jnp.repeat(convolve(next_read, read_kernel).reshape(SEQUENCE_TOTAL, DRAFT_TOKENS, G, N), HEAD_TOTAL // G, axis=2)
    step_sizes = jax.nn.softplus(step_raw.reshape(SEQUENCE_TOTAL, DRAFT_TOKENS, HEAD_TOTAL) + step_size_bias)
    retain_logs = -step_sizes * jnp.exp(head_decay_logs) + extra_decay_logs.reshape(SEQUENCE_TOTAL, DRAFT_TOKENS, HEAD_TOTAL)
    carried = cached_state_history[jnp.arange(SEQUENCE_TOTAL, dtype=jnp.int32), accepted]
    states = [carried]
    outputs = []
    for position in range(DRAFT_TOKENS):
        written = (step_sizes[:, position, :, None] * conv_input[:, position])[:, :, :, None]
        carried = jnp.exp(retain_logs[:, position])[:, :, None, None] * carried + written * conv_write[:, position][:, :, None, :]
        states.append(carried)
        outputs.append(lax.optimization_barrier(jnp.sum(carried * conv_read[:, position][:, :, None, :], axis=-1)) + bypass_scale[:, None] * conv_input[:, position])
    head_out = jnp.stack(outputs, axis=1).reshape(TOKENS, HEAD_TOTAL * P_SIZE)
    gated = (head_out * jax.nn.silu(fresh_gate.astype(jnp.float32))).reshape(TOKENS, G, -1)
    gated = gated * lax.rsqrt(lax.optimization_barrier(jnp.mean(gated * gated, axis=-1, keepdims=True)) + epsilon)
    normed = (gated.reshape(TOKENS, HEAD_TOTAL * P_SIZE) * output_norm_gain).astype(jnp.bfloat16)
    span = HEAD_TOTAL * P_SIZE // N_TP
    total = jnp.zeros((TOKENS, D), jnp.float32)
    for block_index in range(N_TP):
        partial_value = jnp.dot(normed[:, block_index * span:(block_index + 1) * span], output_matrix[block_index * span:(block_index + 1) * span], preferred_element_type=jnp.float32)
        total = total + partial_value.astype(jnp.bfloat16).astype(jnp.float32)
    mixer_out = total.astype(jnp.bfloat16)
    next_states = jnp.stack(states, axis=1)
    return (mixer_out, next_states, next_input, next_write, next_read)
```

```python
import functools

import jax
import jax.numpy as jnp
from jax import lax
from jax.experimental import pallas as pl
from jax.experimental.pallas import tpu as pltpu
from jax.sharding import PartitionSpec as P

D = 4096
HEAD_TOTAL = 64
P_SIZE = 64
N = 128
G = 8
TAPS = 4
DRAFT_TOKENS = 5
KEPT = TAPS - 1
epsilon = 1e-05

F32 = jnp.float32
BF16 = jnp.bfloat16
HIGHEST = lax.Precision.HIGHEST
VMEM_SPEC = pl.BlockSpec(memory_space=pltpu.VMEM)
HBM_SPEC = pl.BlockSpec(memory_space=pltpu.HBM)

COLUMN_TILES = 10
MISC_ROW = 16 * COLUMN_TILES
HALF_ROW = MISC_ROW + 16
BLOCK_ROWS = HALF_ROW + 8 * (COLUMN_TILES // 2)
NORMED_HALF_ROW = 64
NORMED_ROWS = 80


def nt(a, b, precision=None):
    return lax.dot_general(a, b, (((1,), (1,)), ((), ())), precision=precision, preferred_element_type=F32)


def rows_of(shape, axis):
    return lax.broadcasted_iota(jnp.int32, shape, axis)


def by_head(scalars, lanes):
    value = jnp.zeros(lanes.shape, F32)
    for h in range(8):
        value = jnp.where(lanes // P_SIZE == h, scalars[h], value)
    return value


def project_kernel(
    tokens, gain, w_in, w_gate, w_write, w_read, step_t, accepted, history, bias, decay_logs, bypass,
    saved_input, saved_write, saved_read, k_in, k_write, k_read, extra_t, out_gain, w_out,
    out, carried, rows, pick, to_input, to_write, to_read, to_k_in, to_k_write, to_k_read, to_extra, to_gain, to_w_out,
    here, here_gain, m_in, m_gate, m_write, m_read, step_block, s_accepted, s_bias, s_decay, s_bypass, sems,
):
    kv, tp = lax.axis_index("kv"), lax.axis_index("tp")
    step_source = step_t.at[
        pl.ds(pl.multiple_of(tp * 8, 8), 8), pl.ds(pl.multiple_of(kv * 256, 256), 256)
    ]
    pairs = (
        (accepted, s_accepted),
        (tokens, here),
        (gain, here_gain),
        (w_in, m_in),
        (w_gate, m_gate),
        (w_write, m_write),
        (w_read, m_read),
        (step_source, step_block.at[pl.ds(0, 8)]),
        (bias, s_bias),
        (decay_logs, s_decay),
        (bypass, s_bypass),
        (saved_input, to_input),
        (saved_write, to_write),
        (saved_read, to_read),
        (k_in, to_k_in),
        (k_write, to_k_write),
        (k_read, to_k_read),
        (extra_t, to_extra),
        (out_gain, to_gain),
        (w_out, to_w_out),
    )
    copies = [pltpu.make_async_copy(a, b, sems.at[k]) for k, (a, b) in enumerate(pairs)]
    for copy in copies:
        copy.start()
    step_block[8:, :] = jnp.zeros((120, 256), BF16)
    row = rows_of((320, 320), 0)
    column = rows_of((320, 320), 1)
    source = jnp.where(
        row < 256, (row // 16) * 20 + row % 16, ((row - 256) // 4) * 20 + 16 + row % 4
    )
    order = jnp.where(column == source, 1.0, 0.0).astype(BF16)
    copies[0].wait()
    for s in range(4):
        fetch = pltpu.make_async_copy(history.at[s, s_accepted[s]], carried.at[s], sems.at[len(pairs) + s])
        fetch.start()
        copies.append(fetch)
    copies[1].wait()
    copies[2].wait()
    wide = jnp.dot(order, here[...], preferred_element_type=F32)
    squares = jnp.sum(wide * wide, axis=1, keepdims=True)
    scaled = (wide * here_gain[...]).astype(BF16)
    low = rows_of((8, 8, 128), 1) < 4

    def put(part, first):
        tiles = part.shape[1] // 128
        for k in range(tiles):
            tile = part[:256, 128 * k : 128 * k + 128].astype(BF16)
            spot = 16 * (first + k)
            out[:, :, spot : spot + 16, :] = tile.reshape(8, 2, 16, 128)
        for k in range(0, tiles, 2):
            one = part[256:, 128 * k : 128 * k + 128].reshape(8, 8, 128)
            two = part[256:, 128 * k + 128 : 128 * k + 256].reshape(8, 8, 128)
            spot = HALF_ROW + 4 * (first + k)
            out[:, 0, spot : spot + 8, :] = jnp.where(low, one, pltpu.roll(two, 4, 1)).astype(BF16)
            out[:, 1, spot : spot + 8, :] = jnp.where(low, pltpu.roll(one, 4, 1), two).astype(BF16)

    copies[3].wait()
    put(jnp.dot(scaled, m_in[...], preferred_element_type=F32), 0)
    copies[4].wait()
    put(jnp.dot(scaled, m_gate[...], preferred_element_type=F32), 4)
    copies[5].wait()
    copies[6].wait()
    put(
        jnp.concatenate(
            [
                jnp.dot(scaled, m_write[...], preferred_element_type=F32),
                jnp.dot(scaled, m_read[...], preferred_element_type=F32),
            ],
            axis=1,
        ),
        8,
    )
    copies[7].wait()
    misc = nt(scaled, step_block[...])
    misc = jnp.where(rows_of((320, 128), 1) == 8, squares, misc)
    full = misc[:256].reshape(8, 2, 16, 128)
    half = misc[256:].reshape(8, 8, 128)
    even = pltpu.roll(jnp.where(low, half, 0.0), 64, 2)
    odd = pltpu.roll(jnp.where(low, pltpu.roll(half, 4, 1), 0.0), 64, 2)
    out[:, 0, MISC_ROW : MISC_ROW + 16, :] = jnp.concatenate(
        [full[:, 0, :8] + even, full[:, 0, 8:]], axis=1
    ).astype(BF16)
    out[:, 1, MISC_ROW : MISC_ROW + 16, :] = jnp.concatenate(
        [full[:, 1, :8] + odd, full[:, 1, 8:]], axis=1
    ).astype(BF16)
    pick_row, pick_column = rows_of((32, 32), 0), rows_of((32, 32), 1)
    start = jnp.zeros((32, 32), jnp.int32)
    for s in range(4):
        start = jnp.where(pick_row // 8 == s, s_accepted[s] + 8 * s, start)
    pick[...] = jnp.where(
        (pick_row % 8 < KEPT) & (pick_column == start + pick_row % 8), 1.0, 0.0
    ).astype(BF16)
    for copy in copies[8:]:
        copy.wait()
    lanes = rows_of((8, 512), 1)
    rows[0] = by_head(s_bias, lanes)
    rows[1] = jnp.exp(by_head(s_decay, lanes))
    rows[2] = by_head(s_bypass, lanes)


def to_windows(first, second, half, half_high):
    row = rows_of(first.shape, 0)
    last = half if half_high else pltpu.roll(half, 4, 0)
    tiles = (
        pltpu.roll(first, 3, 0),
        jnp.where(row < 6, pltpu.roll(first, 6, 0), pltpu.roll(second, 6, 0)),
        pltpu.roll(second, 1, 0),
        jnp.where(row < 4, pltpu.roll(second, 4, 0), last),
    )
    return jnp.concatenate([jnp.where(row >= KEPT, t, 0.0) for t in tiles], axis=0)


def mix_kernel(
    received, carried, rows, pick, saved_input, saved_write, saved_read, k_in, k_write, k_read, extra_t, out_gain,
    copies, windows, step_x, keeps, writes,
):
    total = received[0].astype(F32)
    for k in range(1, 16):
        total = total + received[k].astype(F32)

    misc = total[MISC_ROW : MISC_ROW + 16]
    misc = to_windows(misc[:8], misc[8:], pltpu.roll(misc[:8], 64, 1), False)
    inverse = lax.rsqrt(misc[:, 8:9] / D + epsilon)

    def fresh(c):
        q = HALF_ROW + 8 * (c // 2)
        tile = to_windows(
            total[16 * c : 16 * c + 8], total[16 * c + 8 : 16 * c + 16], total[q : q + 8], c % 2 == 1
        )
        return (tile * inverse).astype(BF16)

    def joined(first, count):
        return jnp.concatenate([fresh(c) for c in range(first, first + count)], axis=1).astype(F32)

    def window(saved, first, count):
        flat = saved[...].reshape(32, 128 * count)
        return jnp.dot(pick[...], flat, preferred_element_type=F32) + joined(first, count)

    def convolve(value, taps):
        result = value * taps[KEPT : KEPT + 1, :]
        for k in range(KEPT):
            result = result + pltpu.roll(value, KEPT - k, 0) * taps[k : k + 1, :]
        return result * jax.nn.sigmoid(result)

    window_input = window(saved_input, 0, 4)
    window_write = window(saved_write, 8, 1)
    window_read = window(saved_read, 9, 1)
    gate = joined(4, 4)
    windows[:, :512] = window_input.astype(BF16)
    windows[:, 512:640] = window_write.astype(BF16)
    windows[:, 640:] = window_read.astype(BF16)
    conv_input = convolve(window_input, k_in)
    conv_write = convolve(window_write, k_write)
    conv_read = convolve(window_read, k_read)

    spread = jnp.where(
        rows_of((128, 512), 0) == rows_of((128, 512), 1) // P_SIZE, 1.0, 0.0
    )
    row8 = rows_of((32, 512), 0) % 8
    live = row8 >= KEPT
    step_raw = jnp.dot(misc, spread, precision=HIGHEST, preferred_element_type=F32) * inverse
    step = jnp.where(live, jax.nn.softplus(step_raw + rows[0, :1]), 0.0)
    token_row, token = rows_of((32, 20), 0), rows_of((32, 20), 1)
    place = jnp.where(
        (token_row % 8 >= KEPT) & (token == (token_row // 8) * 5 + token_row % 8 - KEPT), 1.0, 0.0
    )
    extra = jnp.dot(
        nt(place, extra_t[...], HIGHEST), spread[:8], precision=HIGHEST, preferred_element_type=F32
    )
    log_keep = jnp.where(live, extra - step * rows[1, :1], 0.0)
    total_log = log_keep + pltpu.roll(log_keep, 1, 0)
    total_log = jnp.where(live, total_log, 0.0)
    total_log = total_log + pltpu.roll(total_log, 2, 0)
    total_log = jnp.where(live, total_log, 0.0)
    total_log = total_log + jnp.where(row8 == 7, pltpu.roll(total_log, 4, 0), 0.0)
    scaled_x = step * conv_input
    step_x[...] = scaled_x
    keeps[...] = jnp.exp(log_keep)
    writes[...] = conv_write

    skip = rows[2, :1] * conv_input
    gate = gate * jax.nn.sigmoid(gate)
    tile_row = rows_of((8, 512), 0)
    normed = []
    for s in range(4):
        at = slice(8 * s, 8 * s + 8)
        logs, x, read = total_log[at], scaled_x[at], conv_read[at]
        weight = nt(read, conv_write[at], HIGHEST)
        value = skip[at]
        for i in range(KEPT, 8):
            keep = jnp.exp(jnp.minimum(logs - logs[i : i + 1], 0.0))
            term = weight[:, i : i + 1] * keep * x[i : i + 1]
            value = value + jnp.where(tile_row >= i, term, 0.0)
        state = carried[s].reshape(512, N).astype(BF16)
        value = value + jnp.exp(logs) * nt(read.astype(BF16), state)
        gated = value * gate[at]
        gated = gated * lax.rsqrt(jnp.mean(gated * gated, axis=1, keepdims=True) + epsilon)
        normed.append(gated * out_gain[...])

    first = jnp.where(tile_row < 5, pltpu.roll(normed[0], 5, 0), pltpu.roll(normed[1], 2, 0))
    last = pltpu.roll(normed[3], 4, 0)
    second = jnp.where(tile_row < 2, pltpu.roll(normed[1], 2, 0), pltpu.roll(normed[2], 7, 0))
    second = jnp.where(tile_row < 7, second, last)
    both = jnp.concatenate([first, second], axis=0).astype(BF16)
    block = [both[:, 128 * c : 128 * c + 128] for c in range(4)]
    for q in range(2):
        low = last[:, 256 * q : 256 * q + 128]
        high = normed[3][:, 256 * q + 128 : 256 * q + 256]
        block.append(jnp.where(tile_row[:, :128] < 4, low, high).astype(BF16))
    block = jnp.concatenate(block, axis=0)
    copies[...] = jnp.broadcast_to(block[None], copies.shape)


def state_kernel(
    carried, windows, step_x, keeps, writes, states, next_in, next_write, next_read,
    held, held_in, held_write, held_read, sems,
):
    copies = []

    def send(source, target):
        copy = pltpu.make_async_copy(source, target, sems.at[len(copies)])
        copy.start()
        copies.append(copy)

    for s in range(4):
        at = pl.ds(8 * s, 8)
        x = step_x[at, :].T
        for h in range(8):
            state = carried[s, h]
            held[s, 0, h] = state
            for r in range(KEPT, 8):
                keep = jnp.broadcast_to(
                    keeps[8 * s + r : 8 * s + r + 1, P_SIZE * h : P_SIZE * h + 1], (P_SIZE, N)
                )
                state = keep * state + x[P_SIZE * h : P_SIZE * h + P_SIZE, r : r + 1] * writes[8 * s + r : 8 * s + r + 1, :]
                held[s, r - KEPT + 1, h] = state
        held_in[s] = windows[at, :512]
        held_write[s] = windows[at, 512:640]
        held_read[s] = windows[at, 640:]
        send(held.at[s], states.at[s])
    send(held_in, next_in)
    send(held_write, next_write)
    send(held_read, next_read)
    for copy in copies:
        copy.wait()


def output_kernel(received, matrix, after, out):
    del after
    left = jnp.concatenate(
        [received[:, 16 * c : 16 * c + 16, :].reshape(256, 128) for c in range(4)], axis=1
    )
    full = jnp.dot(left, matrix[...], preferred_element_type=F32)
    halves = [
        received[:, NORMED_HALF_ROW + 8 * q : NORMED_HALF_ROW + 8 * q + 8, :].reshape(128, 128)
        for q in range(2)
    ]
    left = jnp.concatenate(halves, axis=1)
    low = jnp.dot(left, jnp.concatenate([matrix[0:128], matrix[256:384]], axis=0), preferred_element_type=F32)
    high = jnp.dot(left, jnp.concatenate([matrix[128:256], matrix[384:512]], axis=0), preferred_element_type=F32)
    half = low.reshape(16, 8, 256) + pltpu.roll(high.reshape(16, 8, 256), 4, 1)
    half = half.reshape(8, 2, 8, 256)
    tail = jnp.where(rows_of((8, 8, 256), 1) < 4, half[:, 0], pltpu.roll(half[:, 1], 4, 1))
    out[:, :32, :] = full.reshape(8, 32, 256).astype(BF16)
    out[:, 32:, :] = tail.astype(BF16)


def sum_kernel(received, out):
    total = received[0].astype(F32)
    for k in range(1, 8):
        total = total + received[k].astype(F32)
    low = rows_of((8, 256), 0) < 4
    third, fourth, half = pltpu.roll(total[16:24], 4, 0), pltpu.roll(total[24:32], 4, 0), total[32:]
    out[...] = jnp.concatenate(
        [
            total[:16],
            jnp.where(low, half, third),
            jnp.where(low, third, fourth),
            jnp.where(low, fourth, half),
        ],
        axis=0,
    ).astype(BF16)


def exchange(value, axis):
    return lax.all_to_all(value, axis, 0, 0, tiled=True)


def per_device(
    tokens,
    input_norm_gain,
    input_matrix,
    gate_matrix,
    write_matrix,
    read_matrix,
    step_matrix,
    input_kernel,
    write_kernel,
    read_kernel,
    step_size_bias,
    head_decay_logs,
    bypass_scale,
    extra_decay_logs,
    output_norm_gain,
    output_matrix,
    cached_state_history,
    cached_input_rows,
    cached_write_rows,
    cached_read_rows,
    accepted,
):
    bf16_of = functools.partial(jax.ShapeDtypeStruct, dtype=BF16)
    f32_of = functools.partial(jax.ShapeDtypeStruct, dtype=F32)
    sent, carried, rows, pick, *kept, matrix = pl.pallas_call(
        project_kernel,
        out_shape=(
            bf16_of((8, 2, BLOCK_ROWS, 128)),
            f32_of((4, 8, P_SIZE, N)),
            f32_of((3, 8, 512)),
            bf16_of((32, 32)),
            bf16_of((4, 8, 512)),
            bf16_of((4, 8, N)),
            bf16_of((4, 8, N)),
            f32_of((TAPS, 512)),
            f32_of((TAPS, N)),
            f32_of((TAPS, N)),
            f32_of((8, 20)),
            f32_of((1, 512)),
            bf16_of((512, 256)),
        ),
        in_specs=[HBM_SPEC] * 21,
        out_specs=(VMEM_SPEC,) * 13,
        scratch_shapes=[
            pltpu.VMEM((320, 256), BF16),
            pltpu.VMEM((1, 256), F32),
            pltpu.VMEM((256, 512), BF16),
            pltpu.VMEM((256, 512), BF16),
            pltpu.VMEM((256, 128), BF16),
            pltpu.VMEM((256, 128), BF16),
            pltpu.VMEM((128, 256), BF16),
            pltpu.SMEM((4,), jnp.int32),
            pltpu.SMEM((8,), F32),
            pltpu.SMEM((8,), F32),
            pltpu.SMEM((8,), F32),
            pltpu.SemaphoreType.DMA((24,)),
        ],
        compiler_params=pltpu.CompilerParams(vmem_limit_bytes=16 << 20),
        name="project",
    )(
        *(pltpu.with_memory_space_constraint(a, pltpu.HBM) for a in (
        tokens,
        input_norm_gain.reshape(1, 256),
        input_matrix,
        gate_matrix,
        write_matrix,
        read_matrix,
        step_matrix.T,
        accepted,
        cached_state_history,
        step_size_bias,
        head_decay_logs,
        bypass_scale,
        cached_input_rows,
        cached_write_rows,
        cached_read_rows,
        input_kernel,
        write_kernel,
        read_kernel,
        extra_decay_logs.T,
        output_norm_gain.reshape(1, 512),
        output_matrix,
        ))
    )
    received = exchange(sent.reshape(16, BLOCK_ROWS, 128), "kv")
    copies, windows, step_x, keeps, writes = pl.pallas_call(
        mix_kernel,
        out_shape=(
            bf16_of((16, NORMED_ROWS, 128)),
            bf16_of((32, 768)),
            f32_of((32, 512)),
            f32_of((32, 512)),
            f32_of((32, N)),
        ),
        in_specs=[VMEM_SPEC] * 12,
        out_specs=(VMEM_SPEC,) * 5,
        compiler_params=pltpu.CompilerParams(vmem_limit_bytes=16 << 20),
        name="mix",
    )(received, carried, rows, pick, *kept)
    everyone = exchange(copies, "kv")
    next_states, next_input, next_write, next_read = pl.pallas_call(
        state_kernel,
        out_shape=(
            f32_of((4, 6, 8, P_SIZE, N)),
            bf16_of((4, 8, 512)),
            bf16_of((4, 8, N)),
            bf16_of((4, 8, N)),
        ),
        in_specs=[VMEM_SPEC] * 5,
        out_specs=(HBM_SPEC,) * 4,
        scratch_shapes=[
            pltpu.VMEM((4, 6, 8, P_SIZE, N), F32),
            pltpu.VMEM((4, 8, 512), BF16),
            pltpu.VMEM((4, 8, N), BF16),
            pltpu.VMEM((4, 8, N), BF16),
            pltpu.SemaphoreType.DMA((7,)),
        ],
        compiler_params=pltpu.CompilerParams(vmem_limit_bytes=16 << 20),
        cost_estimate=pl.CostEstimate(flops=200_000_000, bytes_accessed=8_000_000, transcendentals=0),
        name="states",
    )(carried, windows, step_x, keeps, writes)
    partial_sums = pl.pallas_call(
        output_kernel,
        out_shape=jax.ShapeDtypeStruct((8, 40, 256), BF16),
        in_specs=[VMEM_SPEC] * 2 + [HBM_SPEC],
        out_specs=VMEM_SPEC,
        compiler_params=pltpu.CompilerParams(vmem_limit_bytes=8 << 20),
        name="output",
    )(everyone, matrix, pltpu.with_memory_space_constraint(next_write, pltpu.HBM))
    mixer_out = pl.pallas_call(
        sum_kernel,
        out_shape=jax.ShapeDtypeStruct((40, 256), BF16),
        in_specs=[VMEM_SPEC],
        out_specs=VMEM_SPEC,
        compiler_params=pltpu.CompilerParams(vmem_limit_bytes=4 << 20),
        name="total",
    )(exchange(partial_sums, "tp"))
    return (mixer_out, next_states, next_input, next_write, next_read)


def solution(mesh):
    return jax.shard_map(
        per_device,
        mesh=mesh,
        in_specs=(
            P(None, "kv"),
            P("kv"),
            P("kv", "tp"),
            P("kv", "tp"),
            P("kv", "tp"),
            P("kv", "tp"),
            P(),
            P(None, "tp"),
            P(None, "tp"),
            P(None, "tp"),
            P("tp"),
            P("tp"),
            P("tp"),
            P("kv", "tp"),
            P("tp"),
            P("tp", "kv"),
            P("kv", None, "tp", None, None),
            P("kv", None, "tp"),
            P("kv", None, "tp"),
            P("kv", None, "tp"),
            P("kv"),
        ),
        out_specs=(
            P("tp", "kv"),
            P("kv", None, "tp", None, None),
            P("kv", None, "tp"),
            P("kv", None, "tp"),
            P("kv", None, "tp"),
        ),
        check_vma=False,
    )
```

```python
import functools

import jax
import jax.numpy as jnp
from jax import lax
from jax.experimental import pallas as pl
from jax.experimental.pallas import tpu as pltpu
from jax.sharding import PartitionSpec as P

D = 4096
HEAD_TOTAL = 64
P_SIZE = 64
N = 128
G = 8
TAPS = 4
DRAFT_TOKENS = 5
KEPT = TAPS - 1
epsilon = 1e-05

F32 = jnp.float32
BF16 = jnp.bfloat16
HIGHEST = lax.Precision.HIGHEST
VMEM_SPEC = pl.BlockSpec(memory_space=pltpu.VMEM)
HBM_SPEC = pl.BlockSpec(memory_space=pltpu.HBM)

COLUMN_TILES = 10
MISC_ROW = 16 * COLUMN_TILES
HALF_ROW = MISC_ROW + 8
BLOCK_ROWS = HALF_ROW + 8 * (COLUMN_TILES // 2)
NORMED_HALF_ROW = 64
NORMED_ROWS = 80


def nt(a, b, precision=None):
    return lax.dot_general(a, b, (((1,), (1,)), ((), ())), precision=precision, preferred_element_type=F32)


def rows_of(shape, axis):
    return lax.broadcasted_iota(jnp.int32, shape, axis)


def by_head(scalars, lanes):
    value = jnp.zeros(lanes.shape, F32)
    for h in range(8):
        value = jnp.where(lanes // P_SIZE == h, scalars[h], value)
    return value


def project_kernel(
    tokens, gain, w_in, w_gate, w_write, w_read, step_t, accepted, history, bias, decay_logs, bypass,
    saved_input, saved_write, saved_read, k_in, k_write, k_read, extra_t, out_gain, w_out,
    out, carried, rows, pick, to_input, to_write, to_read, to_k_in, to_k_write, to_k_read, to_extra, to_gain, to_w_out,
    here, here_gain, m_in, m_gate, m_write, m_read, step_block, s_accepted, s_bias, s_decay, s_bypass, sems,
):
    kv, tp = lax.axis_index("kv"), lax.axis_index("tp")
    step_source = step_t.at[
        pl.ds(pl.multiple_of(tp * 8, 8), 8), pl.ds(pl.multiple_of(kv * 256, 256), 256)
    ]
    pairs = (
        (accepted, s_accepted),
        (tokens, here),
        (gain, here_gain),
        (w_in, m_in),
        (w_gate, m_gate),
        (w_write, m_write),
        (w_read, m_read),
        (step_source, step_block.at[pl.ds(0, 8)]),
        (bias, s_bias),
        (decay_logs, s_decay),
        (bypass, s_bypass),
        (saved_input, to_input),
        (saved_write, to_write),
        (saved_read, to_read),
        (k_in, to_k_in),
        (k_write, to_k_write),
        (k_read, to_k_read),
        (extra_t, to_extra),
        (out_gain, to_gain),
        (w_out, to_w_out),
    )
    copies = [pltpu.make_async_copy(a, b, sems.at[k]) for k, (a, b) in enumerate(pairs)]
    for copy in copies:
        copy.start()
    step_block[8:, :] = jnp.zeros((120, 256), BF16)
    copies[0].wait()
    for s in range(4):
        fetch = pltpu.make_async_copy(history.at[s, s_accepted[s]], carried.at[s], sems.at[len(pairs) + s])
        fetch.start()
        copies.append(fetch)
    copies[1].wait()
    copies[2].wait()
    wide = here[...].astype(F32)
    squares = jnp.sum(wide * wide, axis=1, keepdims=True)
    scaled = (wide * here_gain[...]).astype(BF16)
    low = rows_of((8, 8, 128), 1) < 4

    def tiles_of(part):
        a, b, c, d, e = (part.reshape(8, 5, 8, 128)[:, k] for k in range(5))
        middle, last = pltpu.roll(d, 4, 1), pltpu.roll(e, 4, 1)
        turned = pltpu.roll(c, 4, 1)
        return (a, b, c, turned), (jnp.where(low, turned, middle), jnp.where(low, middle, last), last, e)

    def put(part, first):
        sets = [tiles_of(part[:, 128 * k : 128 * k + 128]) for k in range(part.shape[1] // 128)]
        for odd in range(2):
            for k, both in enumerate(sets):
                spot = 16 * (first + k)
                out[:, odd, spot : spot + 16, :] = jnp.concatenate(both[odd][:2], axis=1).astype(BF16)
            for k in range(0, len(sets), 2):
                spot = HALF_ROW + 4 * (first + k)
                half = jnp.where(low, sets[k][odd][2], sets[k + 1][odd][3])
                out[:, odd, spot : spot + 8, :] = half.astype(BF16)

    copies[3].wait()
    put(jnp.dot(scaled, m_in[...], preferred_element_type=F32), 0)
    copies[4].wait()
    put(jnp.dot(scaled, m_gate[...], preferred_element_type=F32), 4)
    copies[5].wait()
    copies[6].wait()
    put(
        jnp.concatenate(
            [
                jnp.dot(scaled, m_write[...], preferred_element_type=F32),
                jnp.dot(scaled, m_read[...], preferred_element_type=F32),
            ],
            axis=1,
        ),
        8,
    )
    copies[7].wait()
    misc = nt(scaled, step_block[...])
    misc = jnp.where(rows_of((320, 128), 1) == 8, squares, misc)
    for odd, (one, two, half, _) in enumerate(tiles_of(jnp.where(rows_of((320, 128), 1) < 9, misc, 0.0))):
        value = one + pltpu.roll(two, 32, 2) + jnp.where(low, pltpu.roll(half, 64, 2), 0.0)
        out[:, odd, MISC_ROW : MISC_ROW + 8, :] = value.astype(BF16)
    pick_row, pick_column = rows_of((32, 32), 0), rows_of((32, 32), 1)
    start = jnp.zeros((32, 32), jnp.int32)
    for s in range(4):
        start = jnp.where(pick_row // 8 == s, s_accepted[s] + 8 * s, start)
    pick[...] = jnp.where(
        (pick_row % 8 < KEPT) & (pick_column == start + pick_row % 8), 1.0, 0.0
    ).astype(BF16)
    for copy in copies[8:]:
        copy.wait()
    lanes = rows_of((8, 512), 1)
    rows[0] = by_head(s_bias, lanes)
    rows[1] = jnp.exp(by_head(s_decay, lanes))
    rows[2] = by_head(s_bypass, lanes)


def to_windows(first, second, half, half_high):
    row = rows_of(first.shape, 0)
    last = half if half_high else pltpu.roll(half, 4, 0)
    tiles = (
        pltpu.roll(first, 3, 0),
        jnp.where(row < 6, pltpu.roll(first, 6, 0), pltpu.roll(second, 6, 0)),
        pltpu.roll(second, 1, 0),
        jnp.where(row < 4, pltpu.roll(second, 4, 0), last),
    )
    return jnp.concatenate([jnp.where(row >= KEPT, t, 0.0) for t in tiles], axis=0)


def mix_kernel(
    received, carried, rows, pick, saved_input, saved_write, saved_read, k_in, k_write, k_read, extra_t, out_gain,
    copies, windows, step_x, keeps, writes,
):
    total = received[0].astype(F32)
    for k in range(1, 16):
        total = total + received[k].astype(F32)

    misc = total[MISC_ROW : MISC_ROW + 8]
    misc = to_windows(misc, pltpu.roll(misc, 96, 1), pltpu.roll(misc, 64, 1), False)
    inverse = lax.rsqrt(misc[:, 8:9] / D + epsilon)

    def fresh(c):
        q = HALF_ROW + 8 * (c // 2)
        tile = to_windows(
            total[16 * c : 16 * c + 8], total[16 * c + 8 : 16 * c + 16], total[q : q + 8], c % 2 == 1
        )
        return (tile * inverse).astype(BF16)

    def joined(first, count):
        return jnp.concatenate([fresh(c) for c in range(first, first + count)], axis=1).astype(F32)

    def window(saved, first, count):
        flat = saved[...].reshape(32, 128 * count)
        return jnp.dot(pick[...], flat, preferred_element_type=F32) + joined(first, count)

    def convolve(value, taps):
        result = value * taps[KEPT : KEPT + 1, :]
        for k in range(KEPT):
            result = result + pltpu.roll(value, KEPT - k, 0) * taps[k : k + 1, :]
        return result * jax.nn.sigmoid(result)

    window_input = window(saved_input, 0, 4)
    window_write = window(saved_write, 8, 1)
    window_read = window(saved_read, 9, 1)
    gate = joined(4, 4)
    windows[:, :512] = window_input.astype(BF16)
    windows[:, 512:640] = window_write.astype(BF16)
    windows[:, 640:] = window_read.astype(BF16)
    conv_input = convolve(window_input, k_in)
    conv_write = convolve(window_write, k_write)
    conv_read = convolve(window_read, k_read)

    spread = jnp.where(
        rows_of((128, 512), 0) == rows_of((128, 512), 1) // P_SIZE, 1.0, 0.0
    )
    row8 = rows_of((32, 512), 0) % 8
    live = row8 >= KEPT
    step_raw = jnp.dot(misc, spread, precision=HIGHEST, preferred_element_type=F32) * inverse
    step = jnp.where(live, jax.nn.softplus(step_raw + rows[0, :1]), 0.0)
    token_row, token = rows_of((32, 20), 0), rows_of((32, 20), 1)
    place = jnp.where(
        (token_row % 8 >= KEPT) & (token == (token_row // 8) * 5 + token_row % 8 - KEPT), 1.0, 0.0
    )
    extra = jnp.dot(
        nt(place, extra_t[...], HIGHEST), spread[:8], precision=HIGHEST, preferred_element_type=F32
    )
    log_keep = jnp.where(live, extra - step * rows[1, :1], 0.0)
    total_log = log_keep + pltpu.roll(log_keep, 1, 0)
    total_log = jnp.where(live, total_log, 0.0)
    total_log = total_log + pltpu.roll(total_log, 2, 0)
    total_log = jnp.where(live, total_log, 0.0)
    total_log = total_log + jnp.where(row8 == 7, pltpu.roll(total_log, 4, 0), 0.0)
    scaled_x = step * conv_input
    step_x[...] = scaled_x
    keeps[...] = jnp.exp(log_keep)
    writes[...] = conv_write

    skip = rows[2, :1] * conv_input
    gate = gate * jax.nn.sigmoid(gate)
    tile_row = rows_of((8, 512), 0)
    normed = []
    for s in range(4):
        at = slice(8 * s, 8 * s + 8)
        logs, x, read = total_log[at], scaled_x[at], conv_read[at]
        weight = nt(read, conv_write[at], HIGHEST)
        value = skip[at]
        for i in range(KEPT, 8):
            keep = jnp.exp(jnp.minimum(logs - logs[i : i + 1], 0.0))
            term = weight[:, i : i + 1] * keep * x[i : i + 1]
            value = value + jnp.where(tile_row >= i, term, 0.0)
        state = carried[s].reshape(512, N).astype(BF16)
        value = value + jnp.exp(logs) * nt(read.astype(BF16), state)
        gated = value * gate[at]
        gated = gated * lax.rsqrt(jnp.mean(gated * gated, axis=1, keepdims=True) + epsilon)
        normed.append(gated * out_gain[...])

    first = jnp.where(tile_row < 5, pltpu.roll(normed[0], 5, 0), pltpu.roll(normed[1], 2, 0))
    last = pltpu.roll(normed[3], 4, 0)
    second = jnp.where(tile_row < 2, pltpu.roll(normed[1], 2, 0), pltpu.roll(normed[2], 7, 0))
    second = jnp.where(tile_row < 7, second, last)
    both = jnp.concatenate([first, second], axis=0).astype(BF16)
    block = [both[:, 128 * c : 128 * c + 128] for c in range(4)]
    for q in range(2):
        low = last[:, 256 * q : 256 * q + 128]
        high = normed[3][:, 256 * q + 128 : 256 * q + 256]
        block.append(jnp.where(tile_row[:, :128] < 4, low, high).astype(BF16))
    block = jnp.concatenate(block, axis=0)
    copies[...] = jnp.broadcast_to(block[None], copies.shape)


def in_pieces(value):
    first = value.astype(BF16).astype(F32)
    return first, value - first


def state_kernel(
    carried, windows, step_x, keeps, writes, states, next_in, next_write, next_read,
    held, held_in, held_write, held_read, sems,
):
    copies = []

    def send(source, target):
        copy = pltpu.make_async_copy(source, target, sems.at[len(copies)])
        copy.start()
        copies.append(copy)

    for s in range(4):
        send(carried.at[s], states.at[s, 0])
    row, column = rows_of((8, DRAFT_TOKENS * N), 0), rows_of((8, DRAFT_TOKENS * N), 1)
    own = row == column // N + KEPT
    for s in range(4):
        at = pl.ds(8 * s, 8)
        x_high, x_low = in_pieces(step_x[at, :])
        w_high, w_low = (
            jnp.where(own, jnp.concatenate([w] * DRAFT_TOKENS, axis=1), 0.0) for w in in_pieces(writes[at, :])
        )
        left = jnp.concatenate([x_high, x_high, x_low], axis=0).T.astype(BF16)
        right = jnp.concatenate([w_high, w_low, w_high], axis=0).astype(BF16)
        added = jnp.dot(left, right, preferred_element_type=F32)
        for h in range(8):
            state = carried[s, h]
            for r in range(DRAFT_TOKENS):
                spot = 8 * s + KEPT + r
                keep = jnp.broadcast_to(keeps[spot : spot + 1, P_SIZE * h : P_SIZE * h + 1], (P_SIZE, N))
                state = keep * state + added[P_SIZE * h : P_SIZE * h + P_SIZE, N * r : N * r + N]
                held[s, r, h] = state
        send(held.at[s], states.at[s, pl.ds(1, DRAFT_TOKENS)])
    for s in range(4):
        at = pl.ds(8 * s, 8)
        held_in[s] = windows[at, :512]
        held_write[s] = windows[at, 512:640]
        held_read[s] = windows[at, 640:]
    send(held_in, next_in)
    send(held_write, next_write)
    send(held_read, next_read)
    for copy in copies:
        copy.wait()


def output_kernel(received, matrix, out):
    left = jnp.concatenate(
        [received[:, 16 * c : 16 * c + 16, :].reshape(256, 128) for c in range(4)], axis=1
    )
    full = jnp.dot(left, matrix[...], preferred_element_type=F32)
    halves = [
        received[:, NORMED_HALF_ROW + 8 * q : NORMED_HALF_ROW + 8 * q + 8, :].reshape(128, 128)
        for q in range(2)
    ]
    left = jnp.concatenate(halves, axis=1)
    low = jnp.dot(left, jnp.concatenate([matrix[0:128], matrix[256:384]], axis=0), preferred_element_type=F32)
    high = jnp.dot(left, jnp.concatenate([matrix[128:256], matrix[384:512]], axis=0), preferred_element_type=F32)
    half = low.reshape(16, 8, 256) + pltpu.roll(high.reshape(16, 8, 256), 4, 1)
    half = half.reshape(8, 2, 8, 256)
    tail = jnp.where(rows_of((8, 8, 256), 1) < 4, half[:, 0], pltpu.roll(half[:, 1], 4, 1))
    out[:, :32, :] = full.reshape(8, 32, 256).astype(BF16)
    out[:, 32:, :] = tail.astype(BF16)


def sum_kernel(received, out):
    total = received[0].astype(F32)
    for k in range(1, 8):
        total = total + received[k].astype(F32)
    low = rows_of((8, 256), 0) < 4
    third, fourth, half = pltpu.roll(total[16:24], 4, 0), pltpu.roll(total[24:32], 4, 0), total[32:]
    out[...] = jnp.concatenate(
        [
            total[:16],
            jnp.where(low, half, third),
            jnp.where(low, third, fourth),
            jnp.where(low, fourth, half),
        ],
        axis=0,
    ).astype(BF16)


def exchange(value, axis):
    return lax.all_to_all(value, axis, 0, 0, tiled=True)


def per_device(
    tokens,
    input_norm_gain,
    input_matrix,
    gate_matrix,
    write_matrix,
    read_matrix,
    step_matrix,
    input_kernel,
    write_kernel,
    read_kernel,
    step_size_bias,
    head_decay_logs,
    bypass_scale,
    extra_decay_logs,
    output_norm_gain,
    output_matrix,
    cached_state_history,
    cached_input_rows,
    cached_write_rows,
    cached_read_rows,
    accepted,
):
    bf16_of = functools.partial(jax.ShapeDtypeStruct, dtype=BF16)
    f32_of = functools.partial(jax.ShapeDtypeStruct, dtype=F32)
    sent, carried, rows, pick, *kept, matrix = pl.pallas_call(
        project_kernel,
        out_shape=(
            bf16_of((8, 2, BLOCK_ROWS, 128)),
            f32_of((4, 8, P_SIZE, N)),
            f32_of((3, 8, 512)),
            bf16_of((32, 32)),
            bf16_of((4, 8, 512)),
            bf16_of((4, 8, N)),
            bf16_of((4, 8, N)),
            f32_of((TAPS, 512)),
            f32_of((TAPS, N)),
            f32_of((TAPS, N)),
            f32_of((8, 20)),
            f32_of((1, 512)),
            bf16_of((512, 256)),
        ),
        in_specs=[HBM_SPEC] * 21,
        out_specs=(VMEM_SPEC,) * 13,
        scratch_shapes=[
            pltpu.VMEM((320, 256), BF16),
            pltpu.VMEM((1, 256), F32),
            pltpu.VMEM((256, 512), BF16),
            pltpu.VMEM((256, 512), BF16),
            pltpu.VMEM((256, 128), BF16),
            pltpu.VMEM((256, 128), BF16),
            pltpu.VMEM((128, 256), BF16),
            pltpu.SMEM((4,), jnp.int32),
            pltpu.SMEM((8,), F32),
            pltpu.SMEM((8,), F32),
            pltpu.SMEM((8,), F32),
            pltpu.SemaphoreType.DMA((24,)),
        ],
        compiler_params=pltpu.CompilerParams(vmem_limit_bytes=16 << 20),
        name="project",
    )(
        *(pltpu.with_memory_space_constraint(a, pltpu.HBM) for a in (
        tokens,
        input_norm_gain.reshape(1, 256),
        input_matrix,
        gate_matrix,
        write_matrix,
        read_matrix,
        step_matrix.T,
        accepted,
        cached_state_history,
        step_size_bias,
        head_decay_logs,
        bypass_scale,
        cached_input_rows,
        cached_write_rows,
        cached_read_rows,
        input_kernel,
        write_kernel,
        read_kernel,
        extra_decay_logs.T,
        output_norm_gain.reshape(1, 512),
        output_matrix,
        ))
    )
    received = exchange(sent.reshape(16, BLOCK_ROWS, 128), "kv")
    copies, windows, step_x, keeps, writes = pl.pallas_call(
        mix_kernel,
        out_shape=(
            bf16_of((16, NORMED_ROWS, 128)),
            bf16_of((32, 768)),
            f32_of((32, 512)),
            f32_of((32, 512)),
            f32_of((32, N)),
        ),
        in_specs=[VMEM_SPEC] * 12,
        out_specs=(VMEM_SPEC,) * 5,
        compiler_params=pltpu.CompilerParams(vmem_limit_bytes=16 << 20),
        name="mix",
    )(received, carried, rows, pick, *kept)
    everyone = exchange(copies, "kv")
    next_states, next_input, next_write, next_read = pl.pallas_call(
        state_kernel,
        out_shape=(
            f32_of((4, 6, 8, P_SIZE, N)),
            bf16_of((4, 8, 512)),
            bf16_of((4, 8, N)),
            bf16_of((4, 8, N)),
        ),
        in_specs=[VMEM_SPEC] * 5,
        out_specs=(HBM_SPEC,) * 4,
        scratch_shapes=[
            pltpu.VMEM((4, DRAFT_TOKENS, 8, P_SIZE, N), F32),
            pltpu.VMEM((4, 8, 512), BF16),
            pltpu.VMEM((4, 8, N), BF16),
            pltpu.VMEM((4, 8, N), BF16),
            pltpu.SemaphoreType.DMA((11,)),
        ],
        compiler_params=pltpu.CompilerParams(vmem_limit_bytes=16 << 20),
        cost_estimate=pl.CostEstimate(flops=200_000_000, bytes_accessed=8_000_000, transcendentals=0),
        name="states",
    )(carried, windows, step_x, keeps, writes)
    partial_sums = pl.pallas_call(
        output_kernel,
        out_shape=jax.ShapeDtypeStruct((8, 40, 256), BF16),
        in_specs=[VMEM_SPEC] * 2,
        out_specs=VMEM_SPEC,
        compiler_params=pltpu.CompilerParams(vmem_limit_bytes=8 << 20),
        name="output",
    )(everyone, matrix)
    mixer_out = pl.pallas_call(
        sum_kernel,
        out_shape=jax.ShapeDtypeStruct((40, 256), BF16),
        in_specs=[VMEM_SPEC],
        out_specs=VMEM_SPEC,
        compiler_params=pltpu.CompilerParams(vmem_limit_bytes=4 << 20),
        name="total",
    )(exchange(partial_sums, "tp"))
    return (mixer_out, next_states, next_input, next_write, next_read)


def solution(mesh):
    return jax.shard_map(
        per_device,
        mesh=mesh,
        in_specs=(
            P(None, "kv"),
            P("kv"),
            P("kv", "tp"),
            P("kv", "tp"),
            P("kv", "tp"),
            P("kv", "tp"),
            P(),
            P(None, "tp"),
            P(None, "tp"),
            P(None, "tp"),
            P("tp"),
            P("tp"),
            P("tp"),
            P("kv", "tp"),
            P("tp"),
            P("tp", "kv"),
            P("kv", None, "tp", None, None),
            P("kv", None, "tp"),
            P("kv", None, "tp"),
            P("kv", None, "tp"),
            P("kv"),
        ),
        out_specs=(
            P("tp", "kv"),
            P("kv", None, "tp", None, None),
            P("kv", None, "tp"),
            P("kv", None, "tp"),
            P("kv", None, "tp"),
        ),
        check_vma=False,
    )
```
